32 devices in a mesh: ep: 8 (over z, x), tp: 4 (over y, core).
Axes of the slice: x: 2, y: 2, z: 4, core: 2. Of those that a mesh axis runs over, the one named last changes fastest.
Arguments:
- q_in: bfloat16 [4096, 1024], P('ep', 'tp'), may hold values from -6 to 6
- k_in: bfloat16 [4096, 256], P('ep'), may hold values from -6 to 6
- v_in: bfloat16 [4096, 256], P('ep'), may hold values from -6 to 6
- q_gain: float32 [64], replicated, may hold values from 0.1 to 1.9
- k_gain: float32 [64], replicated, may hold values from 0.1 to 1.9
- w_out: bfloat16 [1024, 2048], P('tp'), may hold values from -0.1875 to 0.1875
- post_gain: float32 [2048], replicated, may hold values from 0.1 to 1.9
- moe_in: bfloat16 [1024, 2048], P('ep'), may hold values from -6 to 6
- routes: int32 [1024, 2], P('ep'), may hold values from 0 to 7, all different within a row; in each aligned block of 128 rows (0 to 127, 128 to 255, ...) at most 48 rows name the same one
- route_logits: float32 [1024, 2], P('ep'), may hold values from -6 to 6
- pre_gain: float32 [2048], replicated, may hold values from 0.1 to 1.9
- w_gate: bfloat16 [8, 2048, 4096], P('ep', None, 'tp'), may hold values from -0.125 to 0.125
- w_up: bfloat16 [8, 2048, 4096], P('ep', None, 'tp'), may hold values from -0.125 to 0.125
- w_down: bfloat16 [8, 4096, 2048], P('ep', 'tp'), may hold values from -0.125 to 0.125
Outputs:
- attn_out: bfloat16 [4096, 2048], P(('ep', 'tp'))
- moe_out: bfloat16 [1024, 2048], P('ep', 'tp')
The draws below stay inside these ranges and needn't reach their ends.
Inputs may be any that keep to these rules, and one draw needn't show every extreme that they name: `routes`: each row names 2 different experts. Among the rows of one index of ep no expert is named by more than 48 rows, a bound that some block reaches of them.
All inputs are finite; a program needn't handle non-finite values.
Results may differ from the reference program's by a relative error of at most 0.018.
Values may be sent and summed in bfloat16 or wider, within the bound.
A program may use at most 64 MiB of HBM per device.

```python
import math
import jax
import jax.numpy as jnp
import numpy as np
from jax import lax

D = 2048
HEADS = 16
KV_HEADS = 4
HEAD = 64
GRID_W = 128
FFE = 4096
TOP = 2
TOKM_DEV = 128
SEQ = 4096
TOKM = 1024
EXPERTS = 8
HEADS_DEV = 4
FF_DEV = 1024
CAP = 48
N_EP = 8
N_TP = 4


def strengthened(drawn, own_key, source, target, shards_of, factor):
    def block_of(axis_at):
        return (jnp.arange(drawn.shape[axis_at]) // (drawn.shape[axis_at] // shards_of)).reshape((-1,) + (1,) * (drawn.ndim - 1 - axis_at))

    one_side = jax.random.permutation(own_key, shards_of)[block_of(target)]
    far = (block_of(target) + shards_of // 2) % shards_of
    return jnp.where((block_of(source) == one_side) | (block_of(source) == far), factor * drawn, drawn)


def block_levels(key, extent, shards, low, largest):
    factor_of, own = 1.0, jax.random.fold_in(key, 6)
    for dim, shards_of in shards:
        heights = jnp.exp(jax.random.uniform(jax.random.fold_in(own, dim), (shards_of,), jnp.float32, low / len(shards), largest / len(shards)))
        factor_of = factor_of * jnp.repeat(heights, extent[dim] // shards_of).reshape([-1 if axis == dim else 1 for axis in range(len(extent))])
    return factor_of


def assign_block(own_key, own, number, rows, number_of, top, bound, slope):
    order = jax.random.permutation(own_key, number_of)
    heavy_load, usual = load_shares(number_of, rows * top, bound, slope, True), load_shares(number_of, rows * top, bound, slope, False)
    places = jnp.arange(number_of)

    def named(lengths, offset_by):
        used = int((lengths > 0).sum())
        fixed = max(1, used // 4)
        shifted = fixed + (places - fixed + offset_by * (used - fixed)) % max(1, number_of - fixed)
        return jnp.zeros((number_of,), jnp.int32).at[order[jnp.where(places < fixed, places, shifted)]].set(jnp.asarray(lengths, jnp.int32))

    lengths = jnp.where(number % 4 == 0, named(heavy_load, number // 4), named(usual, number - number // 4 - 1))
    mixed = jax.random.permutation(jax.random.fold_in(own, 3), number_of)
    source_of, taker = mixed[0:number_of // 2 * 2:2], mixed[1:number_of // 2 * 2:2]
    margin = jnp.minimum(lengths[source_of] - 1, bound - lengths[taker]) // 2
    margin = jnp.where((source_of == order[0]) | (taker == order[0]) | (lengths[taker] == 0), 0, jnp.maximum(margin, 0))
    shifted = jax.random.randint(jax.random.fold_in(own, 4), (number_of // 2,), 0, 1 << 20) % (margin + 1)
    lengths = lengths.at[source_of].add(-shifted).at[taker].add(shifted)
    labels = jnp.searchsorted(jnp.cumsum(lengths), jnp.arange(rows * top), side="right").astype(jnp.int32)
    grid = labels.reshape(top, rows).T
    grid = grid[jax.random.permutation(jax.random.fold_in(own, 1), rows)]
    offset_by = jax.random.randint(jax.random.fold_in(own, 2), (rows, 1), 0, top)
    return jnp.take_along_axis(grid, (jnp.arange(top)[None, :] + offset_by) % top, axis=1)


def load_shares(number_of, total, limit, slope, full):
    weights = [(1 << 20) // math.isqrt(rank ** slope) + 1 for rank in range(1, number_of + 1)]
    largest = limit if full else min(limit, max(-(-total // number_of), total * weights[0] // sum(weights)))
    least = 1 if total - largest >= number_of - 1 else 0
    given, surplus = [largest] + [least] * (number_of - 1), total - largest - least * (number_of - 1)
    while surplus > 0:
        movable = [i for i in range(1, number_of) if given[i] < largest] or [i for i in range(1, number_of) if given[i] < limit]
        pool, budget = sum([weights[i] for i in movable]), surplus
        for i in movable:
            extra = min(limit - given[i], max(1, budget * weights[i] // pool), surplus)
            given[i] = given[i] + extra
            surplus = surplus - extra
    return np.array(given)


def noise(stream_key, extent, deviation, reach, cuts=(), kind=jnp.bfloat16):
    drawn = deviation * jax.random.normal(stream_key, extent, jnp.float32)
    if cuts:
        drawn = drawn * block_levels(stream_key, extent, cuts, -0.22, 0.18)
    return jnp.clip(drawn, -reach, reach).astype(kind)


def heavy_noise(own_key, dims, deviation, most, pieces, heavy, held_as=jnp.bfloat16):
    result = deviation * jax.random.normal(own_key, dims, jnp.float32)
    if pieces:
        result = result * block_levels(own_key, dims, pieces, -0.22, 0.18)
    return jnp.clip(strengthened(result, jax.random.fold_in(own_key, 3), *heavy), -most, most).astype(held_as)


def setup_inputs(seed: int = 0) -> dict:
    arg_keys = jax.random.split(jax.random.key(seed), 15)
    q_in = noise(arg_keys[0], (SEQ, HEADS * HEAD), 1.0, 6.0, ((0, 8), (1, 4)))
    k_in = noise(arg_keys[1], (SEQ, KV_HEADS * HEAD), 1.0, 6.0, ((0, 8),))
    v_in = noise(arg_keys[2], (SEQ, KV_HEADS * HEAD), 1.0, 6.0, ((0, 8),))
    q_gain = jnp.clip(1.0 + 0.18 * jax.random.normal(arg_keys[3], (HEAD,), jnp.float32), 0.1, 1.9)
    k_gain = jnp.clip(1.0 + 0.18 * jax.random.normal(arg_keys[4], (HEAD,), jnp.float32), 0.1, 1.9)
    w_out = noise(arg_keys[5], (HEADS * HEAD, D), (HEADS * HEAD) ** -0.5, 0.1875, ((0, 4),))
    post_gain = jnp.clip(1.0 + 0.18 * jax.random.normal(arg_keys[6], (D,), jnp.float32), 0.1, 1.9)
    moe_in = noise(arg_keys[7], (TOKM, D), 1.0, 6.0, ((0, 8),))
    routes_keys = jax.random.split(jax.random.fold_in(arg_keys[8], 1), TOKM // TOKM_DEV)
    routes_turns = jax.random.permutation(jax.random.fold_in(arg_keys[8], 3), TOKM // TOKM_DEV)
    routes = jax.vmap(lambda own, number: assign_block(jax.random.fold_in(arg_keys[8], 2), own, number, TOKM_DEV, EXPERTS, TOP, CAP, 2))(routes_keys, routes_turns).reshape((TOKM, TOP))
    route_logits = noise(arg_keys[9], (TOKM, TOP), 1.5, 6.0, ((0, 8),), jnp.float32)
    pre_gain = jnp.clip(1.0 + 0.18 * jax.random.normal(arg_keys[10], (D,), jnp.float32), 0.1, 1.9)
    w_gate = noise(arg_keys[11], (EXPERTS, D, FFE), D ** -0.5, 0.125, ((0, 8), (2, 4)))
    w_up = noise(arg_keys[12], (EXPERTS, D, FFE), D ** -0.5, 0.125, ((0, 8), (2, 4)))
    w_down = heavy_noise(arg_keys[13], (EXPERTS, FFE, D), FFE ** -0.5, 0.125, ((0, 8), (1, 4)), (1, 2, 4, 2.0))
    return {"q_in": q_in, "k_in": k_in, "v_in": v_in, "q_gain": q_gain, "k_gain": k_gain, "w_out": w_out, "post_gain": post_gain, "moe_in": moe_in, "routes": routes, "route_logits": route_logits, "pre_gain": pre_gain, "w_gate": w_gate, "w_up": w_up, "w_down": w_down}


EPSILON = 1e-06
ROPE_BASE = 10000.0

def head_norm(values, gain):
    return values * lax.rsqrt(lax.optimization_barrier(jnp.mean(values * values, axis=-1, keepdims=True)) + EPSILON) * gain

def rotate_half(values, angles):
    quarter = angles.shape[-1]
    first_part = values[..., :quarter]
    second_part = values[..., quarter:]
    cosine = jnp.cos(angles)[:, None, :]
    sine_part = jnp.sin(angles)[:, None, :]
    return jnp.concatenate([first_part * cosine - second_part * sine_part, second_part * cosine + first_part * sine_part], axis=-1)

def grid_rotary(values, offset):
    row_count = values.shape[0]
    head_width = values.shape[-1]
    quarter = head_width // 4
    half_width = head_width // 2
    position = offset + jnp.arange(row_count, dtype=jnp.int32)
    grid_row = (position // GRID_W).astype(jnp.float32)
    grid_col = (position % GRID_W).astype(jnp.float32)
    inverse = ROPE_BASE ** (-jnp.arange(quarter, dtype=jnp.float32) / quarter)
    return jnp.concatenate([rotate_half(values[..., :half_width], grid_row[:, None] * inverse[None, :]), rotate_half(values[..., half_width:], grid_col[:, None] * inverse[None, :])], axis=-1)

def slot_table(route_rows, expert_count, capacity):
    token_count, top_count = route_rows.shape
    flat_routes = route_rows.reshape(-1).astype(jnp.int32)
    one_hot = (flat_routes[:, None] == jnp.arange(expert_count, dtype=jnp.int32)[None, :]).astype(jnp.int32)
    ranked = lax.optimization_barrier(jnp.sum((jnp.cumsum(one_hot, axis=0) - 1) * one_hot, axis=1))
    placed = (flat_routes * capacity + ranked).astype(jnp.int32)
    slot_owner = jnp.full((expert_count * capacity,), token_count * top_count, dtype=jnp.int32)
    slot_owner = slot_owner.at[placed].set(jnp.arange(token_count * top_count, dtype=jnp.int32))
    return (slot_owner, placed)

def mixer_half(q_in, k_in, v_in, q_gain, k_gain, w_out, post_gain):
    queries = head_norm(q_in.astype(jnp.float32).reshape(SEQ, HEADS, HEAD), q_gain.astype(jnp.float32))
    queries = grid_rotary(queries, 0).astype(jnp.bfloat16)
    keys = head_norm(k_in.astype(jnp.float32).reshape(SEQ, KV_HEADS, HEAD), k_gain.astype(jnp.float32))
    keys = grid_rotary(keys, 0).astype(jnp.bfloat16)
    repeat = HEADS // KV_HEADS
    key_float = keys.astype(jnp.float32)
    value_float = v_in.astype(jnp.float32).reshape(SEQ, KV_HEADS, HEAD)
    blocked = queries.reshape(SEQ // 128, 128, KV_HEADS, repeat, HEAD)

    def attend(query_block):
        scores = jnp.einsum('qgrd,kgd->grqk', query_block.astype(jnp.float32), key_float) * HEAD ** (-0.5)
        weights = jnp.exp(scores)
        denominator = lax.optimization_barrier(jnp.sum(weights, axis=-1))
        rounded = lax.optimization_barrier(weights.astype(jnp.bfloat16)).astype(jnp.float32)
        summed = jnp.einsum('grqk,kgd->qgrd', rounded, value_float)
        return (summed / jnp.transpose(denominator, (2, 0, 1))[..., None]).astype(jnp.bfloat16)
    head_out = lax.map(attend, blocked).reshape(SEQ, HEADS * HEAD)
    grouped_out = head_out.reshape(SEQ, N_TP, HEADS_DEV * HEAD)
    grouped_w = w_out.reshape(N_TP, HEADS_DEV * HEAD, D)

    def add_group(running, index):
        term = jnp.dot(grouped_out[:, index], grouped_w[index], preferred_element_type=jnp.float32)
        term = lax.optimization_barrier(term.astype(jnp.bfloat16))
        return (running + term.astype(jnp.float32), None)
    mixed, unused = lax.scan(add_group, jnp.zeros((SEQ, D), jnp.float32), jnp.arange(N_TP, dtype=jnp.int32))
    return head_norm(mixed, post_gain.astype(jnp.float32)).astype(jnp.bfloat16)

def experts_half(moe_in, routes, route_logits, pre_gain, w_gate, w_up, w_down):
    normed = head_norm(moe_in.astype(jnp.float32), pre_gain.astype(jnp.float32)).astype(jnp.bfloat16)
    copy_count = TOKM * TOP
    local_copies = TOKM_DEV * TOP
    padded = jnp.concatenate([normed, jnp.zeros((1, D), normed.dtype)], axis=0)
    blocks = routes.reshape(N_EP, TOKM_DEV, TOP)
    owners, unused = jax.vmap(lambda block_routes: slot_table(block_routes, EXPERTS, CAP))(blocks)
    shift_by = (jnp.arange(N_EP, dtype=jnp.int32) * local_copies)[:, None]
    global_owner = jnp.where(owners < local_copies, owners + shift_by, copy_count).astype(jnp.int32)
    per_expert = global_owner.reshape(N_EP, EXPERTS, CAP).transpose(1, 0, 2).reshape(EXPERTS, N_EP * CAP)

    def one_expert(results, inputs):
        owner_ids, gate_w, up_w, down_w = inputs
        gathered = padded[owner_ids // TOP]
        gate_pre = jnp.dot(gathered, gate_w, preferred_element_type=jnp.float32)
        up_pre = jnp.dot(gathered, up_w, preferred_element_type=jnp.float32)
        hidden = (jax.nn.silu(gate_pre) * up_pre).astype(jnp.bfloat16)
        hidden_groups = hidden.reshape(N_EP * CAP, N_TP, FF_DEV)
        down_groups = down_w.reshape(N_TP, FF_DEV, D)

        def add_group(running, index):
            term = jnp.dot(hidden_groups[:, index], down_groups[index], preferred_element_type=jnp.float32)
            term = lax.optimization_barrier(term.astype(jnp.bfloat16))
            return (running + term.astype(jnp.float32), None)
        combined, unused_out = lax.scan(add_group, jnp.zeros((N_EP * CAP, D), jnp.float32), jnp.arange(N_TP, dtype=jnp.int32))
        return (results.at[owner_ids].set(combined.astype(results.dtype)), None)
    results, unused_all = lax.scan(one_expert, jnp.zeros((copy_count + 1, D), jnp.bfloat16), (per_expert, w_gate, w_up, w_down))
    copies = results[:copy_count].reshape(TOKM, TOP, D).astype(jnp.float32)
    route_weight = jax.nn.softmax(route_logits.astype(jnp.float32), axis=-1)
    return lax.optimization_barrier(jnp.sum(route_weight[..., None] * copies, axis=1)).astype(jnp.bfloat16)

def reference(q_in, k_in, v_in, q_gain, k_gain, w_out, post_gain, moe_in, routes, route_logits, pre_gain, w_gate, w_up, w_down):
    attn_out = mixer_half(q_in, k_in, v_in, q_gain, k_gain, w_out, post_gain)
    moe_out = experts_half(moe_in, routes, route_logits, pre_gain, w_gate, w_up, w_down)
    return (attn_out, moe_out)
```

```python
import functools

import jax
import jax.numpy as jnp
from jax import lax
from jax.experimental import pallas as pl
from jax.experimental.pallas import tpu as pltpu
from jax.sharding import PartitionSpec as P

GRID_W = 128
EPSILON = 1e-06
ROPE_BASE = 10000.0
MESH = pl.DeviceIdType.MESH


def head_norm(values, gain):
    return values * lax.rsqrt(jnp.mean(values * values, axis=-1, keepdims=True) + EPSILON) * gain


def rotate_half(values, angles):
    quarter = angles.shape[-1]
    first_part = values[..., :quarter]
    second_part = values[..., quarter:]
    cosine = jnp.cos(angles)[:, None, :]
    sine_part = jnp.sin(angles)[:, None, :]
    return jnp.concatenate(
        [
            first_part * cosine - second_part * sine_part,
            second_part * cosine + first_part * sine_part,
        ],
        axis=-1,
    )


def grid_rotary(values, offset):
    row_count = values.shape[0]
    head_width = values.shape[-1]
    quarter = head_width // 4
    half_width = head_width // 2
    position = offset + jnp.arange(row_count, dtype=jnp.int32)
    grid_row = (position // GRID_W).astype(jnp.float32)
    grid_col = (position % GRID_W).astype(jnp.float32)
    inverse = ROPE_BASE ** (-jnp.arange(quarter, dtype=jnp.float32) / quarter)
    return jnp.concatenate(
        [
            rotate_half(values[..., :half_width], grid_row[:, None] * inverse[None, :]),
            rotate_half(values[..., half_width:], grid_col[:, None] * inverse[None, :]),
        ],
        axis=-1,
    )


def kernel(
    dims,
    q_ref, pair_ref, outgo_ref, mixw_ref, wout_ref, gain_ref, wg_hbm, wu_hbm, wd_hbm,
    attn_ref, moe_ref,
    wg, wu, wd, kvbuf, vx, acc, arrived, hidden,
    pa, pa_in, pa_red, pa_in2, pm, pm_in, pm_red, pm_in2, summed, ret,
    w_sem, loc_sem, kv_s, kv_r, disp_s, disp_r, rel_s, rel_r, fwd_s,
    a1_s, a1_r, a2_s, a2_r, m1_s, m1_r, m2_s, m2_r, ret_s, ret_r,
):
    n_ep, n_tp, heads, cap = dims
    ny = n_tp // 2
    ep = lax.axis_index("ep")
    tp = lax.axis_index("tp")
    core = lax.rem(tp, 2)
    row = tp // 2
    partner = row * 2 + 1 - core
    rows_kv = pair_ref.shape[0]
    dq = outgo_ref.shape[1]
    slots = outgo_ref.shape[0]
    piece = attn_ref.shape[0]

    def remote(src, dst, ss, rs, e, t):
        return pltpu.make_async_remote_copy(
            src_ref=src, dst_ref=dst, send_sem=ss, recv_sem=rs,
            device_id=(e, t), device_id_type=MESH,
        )

    def ep_at(d):
        return lax.rem(ep + d, n_ep)

    def ep_from(d):
        return lax.rem(ep - d + n_ep, n_ep)

    def same_core(d):
        return lax.rem(row + d, ny) * 2 + core

    def row_from(d):
        return lax.rem(row - d + ny, ny)

    def slot_rows(e):
        return pl.ds(pl.multiple_of(e * cap, cap), cap)

    loads = [
        pltpu.make_async_copy(src, dst, w_sem.at[i])
        for i, (src, dst) in enumerate(((wg_hbm, wg), (wu_hbm, wu), (wd_hbm, wd)))
    ]
    own = pltpu.make_async_copy(
        outgo_ref.at[slot_rows(ep)], arrived.at[tp, slot_rows(ep)], loc_sem.at[0]
    )
    own.start()
    barrier = pltpu.get_barrier_semaphore()
    for d in range(1, n_ep):
        pl.semaphore_signal(barrier, inc=1, device_id=(ep_at(d), tp), device_id_type=MESH)
    for d in range(1, ny):
        pl.semaphore_signal(barrier, inc=1, device_id=(ep, same_core(d)), device_id_type=MESH)
    pl.semaphore_signal(barrier, inc=1, device_id=(ep, partner), device_id_type=MESH)
    pl.semaphore_wait(barrier, n_ep - 1 + ny - 1 + 1)

    disp = [
        remote(outgo_ref.at[slot_rows(ep_at(d))], arrived.at[tp, slot_rows(ep)],
               disp_s.at[d], disp_r.at[d], ep_at(d), tp)
        for d in range(1, n_ep)
    ]
    for copy in disp:
        copy.start()

    def kv_copy(d):
        return remote(pair_ref, kvbuf.at[ep], kv_s.at[d], kv_r.at[d], ep_at(d), tp)

    for d in range(1, n_ep):
        kv_copy(d).start()
    for copy in loads:
        copy.start()

    q_rows = q_ref.shape[0]
    tile = min(256, q_rows)

    def attend(keys_of, first):
        keys = keys_of[...]
        lanes = lax.broadcasted_iota(jnp.int32, keys.shape, 1)
        vx[...] = jnp.where(lanes < keys.shape[1] // 2, jnp.ones_like(keys), keys)

        def one(i, carry):
            for sub in range(2):
                at = pl.ds(pl.multiple_of(i * 2 * tile + sub * tile, tile), tile)
                scores = lax.dot_general(
                    q_ref[at, :], keys_of[...], (((1,), (1,)), ((), ())),
                    preferred_element_type=jnp.float32,
                )
                weights = jnp.exp(scores).astype(jnp.bfloat16)
                term = jnp.dot(weights, vx[...], preferred_element_type=jnp.float32)
                if first:
                    acc[at, :] = term
                else:
                    acc[at, :] += term
            return carry

        lax.fori_loop(0, q_rows // (2 * tile), one, 0)

    attend(pair_ref, True)

    def later(d, carry):
        kv_copy(d).wait_recv()
        attend(kvbuf.at[ep_from(d)], False)
        return carry

    early = max(1, n_ep * 3 // 8)
    late = max(early + 1, n_ep - 1)
    lax.fori_loop(1, early, later, 0)

    own.wait()
    for copy in disp:
        copy.wait_recv()
    relay = [
        remote(arrived.at[tp], arrived.at[tp], rel_s.at[d], rel_r.at[d], ep, same_core(d))
        for d in range(1, ny)
    ]
    cross = [
        remote(arrived.at[row_from(d) * 2 + core], arrived.at[row_from(d) * 2 + core],
               fwd_s.at[d], rel_r.at[ny + d], ep, partner)
        for d in range(ny)
    ]
    for copy in relay:
        copy.start()
    cross[0].start()
    lax.fori_loop(early, late, later, 0)
    for d in range(1, ny):
        relay[d - 1].wait_recv()
        cross[d].start()
    lax.fori_loop(late, n_ep, later, 0)

    outs = []
    tokens = q_rows // heads
    half = acc.shape[1] // 2
    for j in range(n_tp):
        pieces = []
        for h in range(heads):
            a = acc[h * tokens + j * piece : h * tokens + (j + 1) * piece, :]
            pieces.append((a[:, half:] / a[:, :half]).astype(jnp.bfloat16))
        mine = pieces[0] if heads == 1 else jnp.concatenate(pieces, axis=1)
        pa[j % 2, j // 2] = jnp.dot(
            mine, wout_ref[...], preferred_element_type=jnp.float32
        ).astype(jnp.bfloat16)
    a1 = remote(pa.at[1 - core], pa_in, a1_s.at[0], a1_r.at[0], ep, partner)
    a1.start()

    for copy in cross:
        copy.wait_recv()
    loads[0].wait()
    loads[1].wait()
    a1.wait_recv()
    for y in range(ny):
        pa_red[y] = (
            pa[core, y].astype(jnp.float32) + pa_in[y].astype(jnp.float32)
        ).astype(jnp.bfloat16)
    a2 = [
        remote(pa_red.at[lax.rem(row + d, ny)], pa_in2.at[row],
               a2_s.at[d], a2_r.at[d], ep, same_core(d))
        for d in range(1, ny)
    ]
    for copy in a2:
        copy.start()

    ff = hidden.shape[1]
    step = min(256, ff)

    def gated(i, carry):
        at = pl.ds(pl.multiple_of(i * step, step), step)
        gate = jnp.zeros((slots, step), jnp.float32)
        up = jnp.zeros((slots, step), jnp.float32)
        for q in range(n_tp):
            x = arrived[q]
            gate = gate + jnp.dot(x, wg[q * dq : (q + 1) * dq, at], preferred_element_type=jnp.float32)
            up = up + jnp.dot(x, wu[q * dq : (q + 1) * dq, at], preferred_element_type=jnp.float32)
        hidden[:, at] = (gate / (1.0 + jnp.exp(-gate)) * up).astype(jnp.bfloat16)
        return carry

    lax.fori_loop(0, ff // step, gated, 0)
    loads[2].wait()

    def down_for(which):
        def down(y, carry):
            cols = pl.ds(pl.multiple_of((y * 2 + which) * dq, dq), dq)
            pm[which, y] = jnp.dot(
                hidden[...], wd[:, cols], preferred_element_type=jnp.float32
            ).astype(jnp.bfloat16)
            return carry

        lax.fori_loop(0, ny, down, 0)

    m1 = remote(pm.at[1 - core], pm_in, m1_s.at[0], m1_r.at[0], ep, partner)
    down_for(1 - core)
    m1.start()
    down_for(core)
    m1.wait_recv()
    for y in range(ny):
        pm_red[y] = (
            pm[core, y].astype(jnp.float32) + pm_in[y].astype(jnp.float32)
        ).astype(jnp.bfloat16)
    m2 = [
        remote(pm_red.at[lax.rem(row + d, ny)], pm_in2.at[row],
               m2_s.at[d], m2_r.at[d], ep, same_core(d))
        for d in range(1, ny)
    ]
    for copy in m2:
        copy.start()

    for copy in a2:
        copy.wait_recv()
    mixed = pa_red[row].astype(jnp.float32)
    for d in range(1, ny):
        mixed = mixed + pa_in2[row_from(d)].astype(jnp.float32)
    square = jnp.mean(mixed * mixed, axis=-1, keepdims=True)
    attn_ref[...] = (mixed * lax.rsqrt(square + EPSILON) * gain_ref[...]).astype(jnp.bfloat16)

    for copy in m2:
        copy.wait_recv()
    total = pm_red[row].astype(jnp.float32)
    for d in range(1, ny):
        total = total + pm_in2[row_from(d)].astype(jnp.float32)
    summed[...] = total.astype(jnp.bfloat16)
    back = [
        remote(summed.at[slot_rows(ep_at(d))], ret.at[slot_rows(ep)],
               ret_s.at[d], ret_r.at[d], ep_at(d), tp)
        for d in range(1, n_ep)
    ]
    for copy in back:
        copy.start()
    mine = pltpu.make_async_copy(
        summed.at[slot_rows(ep)], ret.at[slot_rows(ep)], loc_sem.at[1]
    )
    mine.start()
    mine.wait()
    for copy in back:
        copy.wait_recv()
    mixw = mixw_ref[...]
    high = mixw.astype(jnp.bfloat16)
    low = (mixw - high.astype(jnp.float32)).astype(jnp.bfloat16)
    moe_ref[...] = (
        jnp.dot(high, ret[...], preferred_element_type=jnp.float32)
        + jnp.dot(low, ret[...], preferred_element_type=jnp.float32)
    ).astype(jnp.bfloat16)

    for copy in disp + relay + cross + [a1] + a2 + [m1] + m2 + back:
        copy.wait_send()

    def kv_done(d, carry):
        kv_copy(d).wait_send()
        return carry

    lax.fori_loop(1, n_ep, kv_done, 0)


def per_device(
    n_ep, n_tp,
    q_in, k_in, v_in, q_gain, k_gain, w_out, post_gain,
    moe_in, routes, route_logits, pre_gain, w_gate, w_up, w_down,
):
    bf16 = jnp.bfloat16
    head = q_gain.shape[0]
    rows = q_in.shape[0]
    heads = q_in.shape[1] // head
    kv_count = k_in.shape[1] // head
    repeat = heads * n_tp // kv_count
    ny = n_tp // 2
    offset = lax.axis_index("ep") * rows
    queries = head_norm(q_in.astype(jnp.float32).reshape(rows, heads, head), q_gain)
    queries = grid_rotary(queries, offset).astype(bf16) * jnp.asarray(head ** (-0.5), bf16)
    queries = jnp.transpose(queries, (1, 0, 2)).reshape(heads * rows, head)
    queries = jnp.concatenate([queries, jnp.zeros_like(queries)], axis=1)
    kv_index = lax.axis_index("tp") * heads // repeat
    keys = lax.dynamic_slice_in_dim(k_in, kv_index * head, head, 1)
    values = lax.dynamic_slice_in_dim(v_in, kv_index * head, head, 1)
    keys = head_norm(keys.astype(jnp.float32)[:, None, :], k_gain)
    keys = grid_rotary(keys, offset)[:, 0, :].astype(bf16)
    paired = jnp.concatenate([keys, values], axis=1)

    tokens, top = routes.shape
    width = moe_in.shape[1]
    dq = width // n_tp
    need = max(2, 3 * top * tokens // (2 * n_ep))
    cap = -(-need // 16) * 16
    slots = n_ep * cap
    x = moe_in.astype(jnp.float32)
    scale = lax.rsqrt(jnp.mean(x * x, axis=-1, keepdims=True) + EPSILON)
    first = lax.axis_index("tp") * dq
    x = lax.dynamic_slice_in_dim(moe_in, first, dq, 1).astype(jnp.float32)
    normed = (x * scale * lax.dynamic_slice_in_dim(pre_gain, first, dq, 0)).astype(bf16)
    slot = jnp.arange(slots, dtype=jnp.int32)[None, :]
    route_weight = jax.nn.softmax(route_logits, axis=-1)
    named = jnp.zeros((tokens, slots), jnp.bool_)
    share = jnp.zeros((tokens, slots), jnp.float32)
    for j in range(top):
        hit = routes[:, j : j + 1] == slot // cap
        named = named | hit
        share = share + jnp.where(hit, route_weight[:, j : j + 1], 0.0)
    earlier = jnp.tril(jnp.ones((tokens, tokens), bf16), -1)
    rank = jnp.dot(earlier, named.astype(bf16), preferred_element_type=jnp.float32)
    placed = named & (rank == (slot % cap).astype(jnp.float32))
    mixw = jnp.where(placed, share, 0.0)
    outgo = lax.dot_general(
        placed.astype(bf16), normed, (((0,), (0,)), ((), ())),
        preferred_element_type=jnp.float32,
    ).astype(bf16)

    piece = rows // n_tp
    ff = w_gate.shape[2]
    dma = pltpu.SemaphoreType.DMA
    vmem = pl.BlockSpec(memory_space=pltpu.VMEM)
    hbm = pl.BlockSpec(memory_space=pl.ANY)
    return pl.pallas_call(
        functools.partial(kernel, (n_ep, n_tp, heads, cap)),
        out_shape=(
            jax.ShapeDtypeStruct((piece, width), bf16),
            jax.ShapeDtypeStruct((tokens, dq), bf16),
        ),
        in_specs=[vmem] * 6 + [hbm] * 3,
        out_specs=(vmem, vmem),
        scratch_shapes=[
            pltpu.VMEM((width, ff), bf16),
            pltpu.VMEM((width, ff), bf16),
            pltpu.VMEM((ff, width), bf16),
            pltpu.VMEM((n_ep, rows, 2 * head), bf16),
            pltpu.VMEM((rows, 2 * head), bf16),
            pltpu.VMEM((heads * rows, 2 * head), jnp.float32),
            pltpu.VMEM((n_tp, slots, dq), bf16),
            pltpu.VMEM((slots, ff), bf16),
            pltpu.VMEM((2, ny, piece, width), bf16),
            pltpu.VMEM((ny, piece, width), bf16),
            pltpu.VMEM((ny, piece, width), bf16),
            pltpu.VMEM((ny, piece, width), bf16),
            pltpu.VMEM((2, ny, slots, dq), bf16),
            pltpu.VMEM((ny, slots, dq), bf16),
            pltpu.VMEM((ny, slots, dq), bf16),
            pltpu.VMEM((ny, slots, dq), bf16),
            pltpu.VMEM((slots, dq), bf16),
            pltpu.VMEM((slots, dq), bf16),
            dma((3,)), dma((2,)),
            dma((n_ep,)), dma((n_ep,)), dma((n_ep,)), dma((n_ep,)),
            dma((ny,)), dma((2 * ny,)), dma((ny,)),
            dma((1,)), dma((1,)), dma((ny,)), dma((ny,)),
            dma((1,)), dma((1,)), dma((ny,)), dma((ny,)),
            dma((n_ep,)), dma((n_ep,)),
        ],
        compiler_params=pltpu.CompilerParams(
            collective_id=0, has_side_effects=True, vmem_limit_bytes=60 * 1024 * 1024
        ),
    )(queries, paired, outgo, mixw, w_out, post_gain[None, :], w_gate[0], w_up[0], w_down[0])


def solution(mesh):
    return jax.shard_map(
        functools.partial(per_device, mesh.shape["ep"], mesh.shape["tp"]),
        mesh=mesh,
        in_specs=(
            P("ep", "tp"),
            P("ep", None),
            P("ep", None),
            P(),
            P(),
            P("tp", None),
            P(),
            P("ep", None),
            P("ep", None),
            P("ep", None),
            P(),
            P("ep", None, "tp"),
            P("ep", None, "tp"),
            P("ep", "tp", None),
        ),
        out_specs=(P(("ep", "tp"), None), P("ep", "tp")),
        check_vma=False,
    )
```

```python
import functools

import jax
import jax.numpy as jnp
from jax import lax
from jax.experimental import pallas as pl
from jax.experimental.pallas import tpu as pltpu
from jax.sharding import PartitionSpec as P

GRID_W = 128
EPSILON = 1e-06
ROPE_BASE = 10000.0
MESH = pl.DeviceIdType.MESH


def head_norm(values, gain):
    return values * lax.rsqrt(jnp.mean(values * values, axis=-1, keepdims=True) + EPSILON) * gain


def rotate_half(values, angles):
    quarter = angles.shape[-1]
    first_part = values[..., :quarter]
    second_part = values[..., quarter:]
    cosine = jnp.cos(angles)[:, None, :]
    sine_part = jnp.sin(angles)[:, None, :]
    return jnp.concatenate(
        [
            first_part * cosine - second_part * sine_part,
            second_part * cosine + first_part * sine_part,
        ],
        axis=-1,
    )


def grid_rotary(values, offset):
    row_count = values.shape[0]
    head_width = values.shape[-1]
    quarter = head_width // 4
    half_width = head_width // 2
    position = offset + jnp.arange(row_count, dtype=jnp.int32)
    grid_row = (position // GRID_W).astype(jnp.float32)
    grid_col = (position % GRID_W).astype(jnp.float32)
    inverse = ROPE_BASE ** (-jnp.arange(quarter, dtype=jnp.float32) / quarter)
    return jnp.concatenate(
        [
            rotate_half(values[..., :half_width], grid_row[:, None] * inverse[None, :]),
            rotate_half(values[..., half_width:], grid_col[:, None] * inverse[None, :]),
        ],
        axis=-1,
    )


def kernel(
    dims,
    q_ref, pair_ref, x_ref, route_ref, logit_ref, pre_ref, ids_ref, wout_ref, gain_ref, wg_hbm, wu_hbm, wd_hbm,
    attn_ref, moe_ref,
    outgo_ref, mixw_ref, wg, wu, wd, kvbuf, vx, acc, arrived, hidden,
    pa, pa_in, pa_red, pa_in2, pm, pm_in, pm_red, pm_in2, summed, ret,
    w_sem, loc_sem, kv_s, kv_r, disp_s, disp_r, rel_s, rel_r, fwd_s,
    a1_s, a1_r, a2_s, a2_r, m1_s, m1_r, m2_s, m2_r, ret_s, ret_r,
):
    n_ep, n_tp, heads, cap = dims
    ny = n_tp // 2
    ep = lax.axis_index("ep")
    tp = lax.axis_index("tp")
    core = lax.rem(tp, 2)
    row = tp // 2
    partner = row * 2 + 1 - core
    rows_kv = pair_ref.shape[0]
    dq = outgo_ref.shape[1]
    slots = outgo_ref.shape[0]
    piece = attn_ref.shape[0]

    def remote(src, dst, ss, rs, e, t):
        return pltpu.make_async_remote_copy(
            src_ref=src, dst_ref=dst, send_sem=ss, recv_sem=rs,
            device_id=(e, t), device_id_type=MESH,
        )

    def ep_at(d):
        return lax.rem(ep + d, n_ep)

    def ep_from(d):
        return lax.rem(ep - d + n_ep, n_ep)

    def same_core(d):
        return lax.rem(row + d, ny) * 2 + core

    def row_from(d):
        return lax.rem(row - d + ny, ny)

    def slot_rows(e):
        return pl.ds(pl.multiple_of(e * cap, cap), cap)

    loads = [
        pltpu.make_async_copy(src, dst, w_sem.at[i])
        for i, (src, dst) in enumerate(((wg_hbm, wg), (wu_hbm, wu), (wd_hbm, wd)))
    ]
    barrier = pltpu.get_barrier_semaphore()
    for d in range(1, n_ep):
        pl.semaphore_signal(barrier, inc=1, device_id=(ep_at(d), tp), device_id_type=MESH)
    for d in range(1, ny):
        pl.semaphore_signal(barrier, inc=1, device_id=(ep, same_core(d)), device_id_type=MESH)
    pl.semaphore_signal(barrier, inc=1, device_id=(ep, partner), device_id_type=MESH)

    x = x_ref[...].astype(jnp.float32)
    scale = lax.rsqrt(jnp.mean(x * x, axis=-1, keepdims=True) + EPSILON)
    mine = pl.ds(pl.multiple_of(tp * dq, dq), dq)
    normed = (x_ref[:, mine].astype(jnp.float32) * scale * pre_ref[:, mine]).astype(jnp.bfloat16)
    logits = logit_ref[...]
    top = logits.shape[1]
    tokens = logits.shape[0]
    power = jnp.exp(logits - jnp.max(logits, axis=1, keepdims=True))
    chance = power / jnp.sum(power, axis=1, keepdims=True)
    named = jnp.zeros((tokens, slots), jnp.float32)
    share = jnp.zeros((tokens, slots), jnp.float32)
    for j in range(top):
        hit = route_ref[:, j : j + 1] == ids_ref[0:1, :]
        named = jnp.where(hit, 1.0, named)
        share = jnp.where(hit, chance[:, j : j + 1], share)
    below = lax.broadcasted_iota(jnp.int32, (tokens, tokens), 1) < lax.broadcasted_iota(
        jnp.int32, (tokens, tokens), 0
    )
    rank = jnp.dot(
        jnp.where(below, 1.0, 0.0).astype(jnp.bfloat16), named.astype(jnp.bfloat16),
        preferred_element_type=jnp.float32,
    )
    placed = jnp.where(rank == ids_ref[1:2, :].astype(jnp.float32), named, 0.0)
    mixw_ref[...] = placed * share
    outgo_ref[...] = lax.dot_general(
        placed.astype(jnp.bfloat16), normed, (((0,), (0,)), ((), ())),
        preferred_element_type=jnp.float32,
    ).astype(jnp.bfloat16)
    own = pltpu.make_async_copy(
        outgo_ref.at[slot_rows(ep)], arrived.at[tp, slot_rows(ep)], loc_sem.at[0]
    )
    own.start()
    pl.semaphore_wait(barrier, n_ep - 1 + ny - 1 + 1)

    disp = [
        remote(outgo_ref.at[slot_rows(ep_at(d))], arrived.at[tp, slot_rows(ep)],
               disp_s.at[d], disp_r.at[d], ep_at(d), tp)
        for d in range(1, n_ep)
    ]
    nz = n_ep // 2
    side = lax.rem(ep, 2)
    col = ep // 2
    mate = col * 2 + 1 - side

    def col_from(d, which):
        return lax.rem(col - d + nz, nz) * 2 + which

    def kv_direct(d):
        return remote(pair_ref, kvbuf.at[ep], kv_s.at[d], kv_r.at[d],
                      lax.rem(col + d, nz) * 2 + side, tp)

    def kv_pass(d):
        held = kvbuf.at[col_from(d, side)]
        return remote(held, held, kv_s.at[nz + d], kv_r.at[nz + d], mate, tp)

    kv_mate = remote(pair_ref, kvbuf.at[ep], kv_s.at[nz], kv_r.at[nz], mate, tp)
    kv_mate.start()
    for copy in disp:
        copy.start()
    for d in range(1, nz):
        kv_direct(d).start()
    for copy in loads:
        copy.start()

    q_rows = q_ref.shape[0]
    tile = min(256, q_rows)

    def attend(keys_of, first):
        keys = keys_of[...]
        lanes = lax.broadcasted_iota(jnp.int32, keys.shape, 1)
        vx[...] = jnp.where(lanes < keys.shape[1] // 2, jnp.ones_like(keys), keys)

        def one(i, carry):
            for sub in range(2):
                at = pl.ds(pl.multiple_of(i * 2 * tile + sub * tile, tile), tile)
                scores = lax.dot_general(
                    q_ref[at, :], keys_of[...], (((1,), (1,)), ((), ())),
                    preferred_element_type=jnp.float32,
                )
                weights = jnp.exp(scores).astype(jnp.bfloat16)
                term = jnp.dot(weights, vx[...], preferred_element_type=jnp.float32)
                if first:
                    acc[at, :] = term
                else:
                    acc[at, :] += term
            return carry

        lax.fori_loop(0, q_rows // (2 * tile), one, 0)

    attend(pair_ref, True)

    kv_mate.wait_recv()
    attend(kvbuf.at[mate], False)

    def later(d, carry):
        kv_direct(d).wait_recv()
        kv_pass(d).start()
        attend(kvbuf.at[col_from(d, side)], False)
        kv_pass(d).wait_recv()
        attend(kvbuf.at[col_from(d, 1 - side)], False)
        return carry

    early = 1 + (nz - 1) // 3
    late = max(early, nz - 1)
    lax.fori_loop(1, early, later, 0)

    own.wait()
    for copy in disp:
        copy.wait_recv()
    relay = [
        remote(arrived.at[tp], arrived.at[tp], rel_s.at[d], rel_r.at[d], ep, same_core(d))
        for d in range(1, ny)
    ]
    cross = [
        remote(arrived.at[row_from(d) * 2 + core], arrived.at[row_from(d) * 2 + core],
               fwd_s.at[d], rel_r.at[ny + d], ep, partner)
        for d in range(ny)
    ]
    for copy in relay:
        copy.start()
    cross[0].start()
    lax.fori_loop(early, late, later, 0)
    for d in range(1, ny):
        relay[d - 1].wait_recv()
        cross[d].start()
    lax.fori_loop(late, nz, later, 0)

    outs = []
    tokens = q_rows // heads
    half = acc.shape[1] // 2
    for j in range(n_tp):
        pieces = []
        for h in range(heads):
            a = acc[h * tokens + j * piece : h * tokens + (j + 1) * piece, :]
            pieces.append((a[:, half:] / a[:, :half]).astype(jnp.bfloat16))
        mine = pieces[0] if heads == 1 else jnp.concatenate(pieces, axis=1)
        pa[j % 2, j // 2] = jnp.dot(
            mine, wout_ref[...], preferred_element_type=jnp.float32
        ).astype(jnp.bfloat16)
    a1 = remote(pa.at[1 - core], pa_in, a1_s.at[0], a1_r.at[0], ep, partner)
    a1.start()

    for copy in cross:
        copy.wait_recv()
    loads[0].wait()
    loads[1].wait()
    a1.wait_recv()
    for y in range(ny):
        pa_red[y] = (
            pa[core, y].astype(jnp.float32) + pa_in[y].astype(jnp.float32)
        ).astype(jnp.bfloat16)
    a2 = [
        remote(pa_red.at[lax.rem(row + d, ny)], pa_in2.at[row],
               a2_s.at[d], a2_r.at[d], ep, same_core(d))
        for d in range(1, ny)
    ]
    for copy in a2:
        copy.start()

    ff = hidden.shape[1]
    step = min(256, ff)

    def gated(i, carry):
        at = pl.ds(pl.multiple_of(i * step, step), step)
        gate = jnp.zeros((slots, step), jnp.float32)
        up = jnp.zeros((slots, step), jnp.float32)
        for q in range(n_tp):
            x = arrived[q]
            gate = gate + jnp.dot(x, wg[q * dq : (q + 1) * dq, at], preferred_element_type=jnp.float32)
            up = up + jnp.dot(x, wu[q * dq : (q + 1) * dq, at], preferred_element_type=jnp.float32)
        hidden[:, at] = (gate / (1.0 + jnp.exp(-gate)) * up).astype(jnp.bfloat16)
        return carry

    lax.fori_loop(0, ff // step, gated, 0)
    loads[2].wait()

    def down_for(which):
        def down(y, carry):
            cols = pl.ds(pl.multiple_of((y * 2 + which) * dq, dq), dq)
            pm[which, y] = jnp.dot(
                hidden[...], wd[:, cols], preferred_element_type=jnp.float32
            ).astype(jnp.bfloat16)
            return carry

        lax.fori_loop(0, ny, down, 0)

    m1 = remote(pm.at[1 - core], pm_in, m1_s.at[0], m1_r.at[0], ep, partner)
    down_for(1 - core)
    m1.start()
    down_for(core)
    m1.wait_recv()
    for y in range(ny):
        pm_red[y] = (
            pm[core, y].astype(jnp.float32) + pm_in[y].astype(jnp.float32)
        ).astype(jnp.bfloat16)
    m2 = [
        remote(pm_red.at[lax.rem(row + d, ny)], pm_in2.at[row],
               m2_s.at[d], m2_r.at[d], ep, same_core(d))
        for d in range(1, ny)
    ]
    for copy in m2:
        copy.start()

    for copy in a2:
        copy.wait_recv()
    mixed = pa_red[row].astype(jnp.float32)
    for d in range(1, ny):
        mixed = mixed + pa_in2[row_from(d)].astype(jnp.float32)
    square = jnp.mean(mixed * mixed, axis=-1, keepdims=True)
    attn_ref[...] = (mixed * lax.rsqrt(square + EPSILON) * gain_ref[...]).astype(jnp.bfloat16)

    for copy in m2:
        copy.wait_recv()
    total = pm_red[row].astype(jnp.float32)
    for d in range(1, ny):
        total = total + pm_in2[row_from(d)].astype(jnp.float32)
    summed[...] = total.astype(jnp.bfloat16)
    back = [
        remote(summed.at[slot_rows(ep_at(d))], ret.at[slot_rows(ep)],
               ret_s.at[d], ret_r.at[d], ep_at(d), tp)
        for d in range(1, n_ep)
    ]
    for copy in back:
        copy.start()
    mine = pltpu.make_async_copy(
        summed.at[slot_rows(ep)], ret.at[slot_rows(ep)], loc_sem.at[1]
    )
    mine.start()
    mine.wait()
    for copy in back:
        copy.wait_recv()
    mixw = mixw_ref[...]
    high = mixw.astype(jnp.bfloat16)
    low = (mixw - high.astype(jnp.float32)).astype(jnp.bfloat16)
    moe_ref[...] = (
        jnp.dot(high, ret[...], preferred_element_type=jnp.float32)
        + jnp.dot(low, ret[...], preferred_element_type=jnp.float32)
    ).astype(jnp.bfloat16)

    for copy in [kv_mate] + disp + relay + cross + [a1] + a2 + [m1] + m2 + back:
        copy.wait_send()

    def kv_done(d, carry):
        kv_direct(d).wait_send()
        kv_pass(d).wait_send()
        return carry

    lax.fori_loop(1, nz, kv_done, 0)


def per_device(
    n_ep, n_tp,
    q_in, k_in, v_in, q_gain, k_gain, w_out, post_gain,
    moe_in, routes, route_logits, pre_gain, w_gate, w_up, w_down,
):
    bf16 = jnp.bfloat16
    head = q_gain.shape[0]
    rows = q_in.shape[0]
    heads = q_in.shape[1] // head
    kv_count = k_in.shape[1] // head
    repeat = heads * n_tp // kv_count
    ny = n_tp // 2
    offset = lax.axis_index("ep") * rows
    queries = head_norm(q_in.astype(jnp.float32).reshape(rows, heads, head), q_gain)
    queries = grid_rotary(queries, offset).astype(bf16) * jnp.asarray(head ** (-0.5), bf16)
    queries = jnp.transpose(queries, (1, 0, 2)).reshape(heads * rows, head)
    queries = jnp.concatenate([queries, jnp.zeros_like(queries)], axis=1)
    kv_index = lax.axis_index("tp") * heads // repeat
    keys = lax.dynamic_slice_in_dim(k_in, kv_index * head, head, 1)
    values = lax.dynamic_slice_in_dim(v_in, kv_index * head, head, 1)
    keys = head_norm(keys.astype(jnp.float32)[:, None, :], k_gain)
    keys = grid_rotary(keys, offset)[:, 0, :].astype(bf16)
    paired = jnp.concatenate([keys, values], axis=1)

    tokens, top = routes.shape
    width = moe_in.shape[1]
    dq = width // n_tp
    need = max(2, 3 * top * tokens // (2 * n_ep))
    cap = -(-need // 16) * 16
    slots = n_ep * cap
    slot = jnp.arange(slots, dtype=jnp.int32)
    ids = jnp.stack([slot // cap, slot % cap])

    piece = rows // n_tp
    ff = w_gate.shape[2]
    dma = pltpu.SemaphoreType.DMA
    vmem = pl.BlockSpec(memory_space=pltpu.VMEM)
    hbm = pl.BlockSpec(memory_space=pl.ANY)
    return pl.pallas_call(
        functools.partial(kernel, (n_ep, n_tp, heads, cap)),
        out_shape=(
            jax.ShapeDtypeStruct((piece, width), bf16),
            jax.ShapeDtypeStruct((tokens, dq), bf16),
        ),
        in_specs=[vmem] * 9 + [hbm] * 3,
        out_specs=(vmem, vmem),
        scratch_shapes=[
            pltpu.VMEM((slots, dq), bf16),
            pltpu.VMEM((tokens, slots), jnp.float32),
            pltpu.VMEM((width, ff), bf16),
            pltpu.VMEM((width, ff), bf16),
            pltpu.VMEM((ff, width), bf16),
            pltpu.VMEM((n_ep, rows, 2 * head), bf16),
            pltpu.VMEM((rows, 2 * head), bf16),
            pltpu.VMEM((heads * rows, 2 * head), jnp.float32),
            pltpu.VMEM((n_tp, slots, dq), bf16),
            pltpu.VMEM((slots, ff), bf16),
            pltpu.VMEM((2, ny, piece, width), bf16),
            pltpu.VMEM((ny, piece, width), bf16),
            pltpu.VMEM((ny, piece, width), bf16),
            pltpu.VMEM((ny, piece, width), bf16),
            pltpu.VMEM((2, ny, slots, dq), bf16),
            pltpu.VMEM((ny, slots, dq), bf16),
            pltpu.VMEM((ny, slots, dq), bf16),
            pltpu.VMEM((ny, slots, dq), bf16),
            pltpu.VMEM((slots, dq), bf16),
            pltpu.VMEM((slots, dq), bf16),
            dma((3,)), dma((2,)),
            dma((n_ep,)), dma((n_ep,)), dma((n_ep,)), dma((n_ep,)),
            dma((ny,)), dma((2 * ny,)), dma((ny,)),
            dma((1,)), dma((1,)), dma((ny,)), dma((ny,)),
            dma((1,)), dma((1,)), dma((ny,)), dma((ny,)),
            dma((n_ep,)), dma((n_ep,)),
        ],
        compiler_params=pltpu.CompilerParams(
            collective_id=0, has_side_effects=True, vmem_limit_bytes=60 * 1024 * 1024
        ),
    )(queries, paired, moe_in, routes, route_logits, pre_gain[None, :], ids, w_out, post_gain[None, :], w_gate[0], w_up[0], w_down[0])


def solution(mesh):
    return jax.shard_map(
        functools.partial(per_device, mesh.shape["ep"], mesh.shape["tp"]),
        mesh=mesh,
        in_specs=(
            P("ep", "tp"),
            P("ep", None),
            P("ep", None),
            P(),
            P(),
            P("tp", None),
            P(),
            P("ep", None),
            P("ep", None),
            P("ep", None),
            P(),
            P("ep", None, "tp"),
            P("ep", None, "tp"),
            P("ep", "tp", None),
        ),
        out_specs=(P(("ep", "tp"), None), P("ep", "tp")),
        check_vma=False,
    )
```
